32 devices in a mesh: sp: 8 (over z, x), tp: 4 (over y, core).
Axes of the slice: x: 2, y: 2, z: 4, core: 2. Of those that a mesh axis runs over, the one named last changes fastest.
Arguments:
- tokens: bfloat16 [8192, 2048], P('sp'), may hold values from -8 to 8
- norm_gain: float32 [2048], replicated, may hold values from 0.1 to 1.9
- query_weight: bfloat16 [2048, 512], P(None, 'tp'), may hold values from -40 to 40
- key_weight: bfloat16 [2048, 256], P(None, 'tp'), may hold values from -1 to 1
- value_weight: bfloat16 [2048, 256], P(None, 'tp'), may hold values from -0.125 to 0.125
- sink_logits: float32 [8], P('tp'), may hold values from 1 to 6
- conv_in_weight: bfloat16 [2048, 512], P(None, 'tp'), may hold values from -0.125 to 0.125
- conv_gate_weight: bfloat16 [2048, 512], P(None, 'tp'), may hold values from -0.125 to 0.125
- conv_taps: bfloat16 [31, 512], replicated, may hold values from -1 to 1
- conv_gain: float32 [512], replicated, may hold values from 0.1 to 1.9
- point_weight: bfloat16 [512, 512], replicated, may hold values from -0.25 to 0.25
- output_gain: float32 [1024], replicated, may hold values from 0.1 to 1.9
- output_weight: bfloat16 [1024, 2048], P('sp'), may hold values from -0.1875 to 0.1875
Outputs:
- mixed_output: bfloat16 [8192, 2048], P(('sp', 'tp'))
The draws below stay inside these ranges and needn't reach their ends.
All inputs are finite; a program needn't handle non-finite values.
Results may differ from the reference program's by a relative error of at most 0.0087.
Values may be sent and summed in bfloat16 or wider, within the bound.
A program may use at most 64 MiB of HBM per device.

```python
import jax
import jax.numpy as jnp
from jax import lax

D = 2048
HEADS = 8
KV_HEADS = 4
HEAD_DIM = 64
CHANNELS = 512
WINDOW = 128
CONV_WIDTH = 31
TOKENS = 8192
MIX = 1024


def base_query(key):
    gaussian = jax.random.normal(jax.random.fold_in(key, 501), (D, HEADS * HEAD_DIM), jnp.float32)
    return jnp.clip(gaussian, -6.0, 6.0) * D ** (-0.5)


def draw_query_weight(key, part):
    unscaled = base_query(key)
    return unscaled.astype(jnp.bfloat16)


def draw_key_weight(key, part):
    fresh_noise = jax.random.normal(jax.random.fold_in(key, 502), (D, KV_HEADS * HEAD_DIM), jnp.float32)
    fresh_noise = jnp.clip(fresh_noise, -6.0, 6.0) * D ** (-0.5)
    return fresh_noise.astype(jnp.bfloat16)


def draw_tokens(key, part):
    shape_rows = (TOKENS, D)
    gaussian = jnp.clip(jax.random.normal(jax.random.fold_in(key, 601), shape_rows, jnp.float32), -6.0, 6.0)
    return gaussian.astype(jnp.bfloat16)


def block_levels(key, extent, split, low, top_value):
    def one(dim, shards_of):
        heights = jax.random.uniform(jax.random.fold_in(jax.random.fold_in(key, 6), dim), (shards_of,), jnp.float32, low / len(split), top_value / len(split))
        return jnp.repeat(jnp.exp(heights), extent[dim] // shards_of).reshape((-1,) + (1,) * (len(extent) - dim - 1))

    factor_of = one(*split[0])
    for cut in split[1:]:
        factor_of = factor_of * one(*cut)
    return factor_of


def scatter_about(key, dims, deviation, reach, cuts=(), kind=jnp.bfloat16):
    entries = deviation * jax.random.normal(key, dims, jnp.float32)
    if cuts:
        entries = entries * block_levels(key, dims, cuts, -0.22, 0.18)
    return jnp.clip(entries, -reach, reach).astype(kind)


def setup_inputs(seed: int = 0) -> dict:
    seeds = jax.random.split(jax.random.key(seed), 14)
    return {
        "tokens": draw_tokens(jax.random.fold_in(seeds[13], 71), 0),
        "norm_gain": jnp.clip(1.0 + 0.18 * jax.random.normal(seeds[1], (D,), jnp.float32), 0.1, 1.9),
        "query_weight": draw_query_weight(jax.random.fold_in(seeds[13], 71), 0),
        "key_weight": draw_key_weight(jax.random.fold_in(seeds[13], 71), 0),
        "value_weight": scatter_about(seeds[4], (D, KV_HEADS * HEAD_DIM), D ** -0.5, 0.125, ((1, 4),)),
        "sink_logits": jnp.clip(1.0 + 5.0 * jax.random.uniform(seeds[5], (HEADS,), jnp.float32) ** block_levels(seeds[5], (HEADS,), ((0, 4),), -0.2, 0.2), 1.0, 6.0),
        "conv_in_weight": scatter_about(seeds[6], (D, CHANNELS), D ** -0.5, 0.125, ((1, 4),)),
        "conv_gate_weight": scatter_about(seeds[7], (D, CHANNELS), D ** -0.5, 0.125, ((1, 4),)),
        "conv_taps": scatter_about(seeds[8], (CONV_WIDTH, CHANNELS), CONV_WIDTH ** -0.5, 1.0),
        "conv_gain": jnp.clip(1.0 + 0.18 * jax.random.normal(seeds[9], (CHANNELS,), jnp.float32), 0.1, 1.9),
        "point_weight": scatter_about(seeds[10], (CHANNELS, CHANNELS), CHANNELS ** -0.5, 0.25),
        "output_gain": jnp.clip(1.0 + 0.18 * jax.random.normal(seeds[11], (MIX,), jnp.float32), 0.1, 1.9),
        "output_weight": scatter_about(seeds[12], (MIX, D), MIX ** -0.5, 0.1875, ((0, 8),)),
    }


NORM_EPSILON = 1e-06
MASKED_SCORE = -1e+30

def rms_rows(values, scale_gain):
    return values * lax.rsqrt(lax.optimization_barrier(jnp.mean(values * values, axis=-1, keepdims=True)) + NORM_EPSILON) * scale_gain

def depthwise(current, earlier_rows, tap_weights):
    extended = jnp.concatenate([earlier_rows, current], axis=0).astype(jnp.float32)
    tap_floats = tap_weights.astype(jnp.float32)
    row_count = current.shape[0]
    result = jnp.zeros(current.shape, jnp.float32)
    for tap_index in range(CONV_WIDTH):
        result = result + tap_floats[tap_index] * extended[tap_index:tap_index + row_count]
    return lax.optimization_barrier(result.astype(jnp.bfloat16))

def layer_activate(conv_rows, channel_gain):
    widened = conv_rows.astype(jnp.float32)
    centered = widened - lax.optimization_barrier(jnp.mean(widened, axis=-1, keepdims=True))
    scaled = centered * lax.rsqrt(lax.optimization_barrier(jnp.mean(centered * centered, axis=-1, keepdims=True)) + NORM_EPSILON) * channel_gain
    return jax.nn.silu(scaled).astype(jnp.bfloat16)

def merge_groups(attended, pointwise, output_gain):
    head_width = attended.shape[1]
    return jnp.concatenate([rms_rows(attended.astype(jnp.float32), output_gain[:head_width]), rms_rows(pointwise, output_gain[head_width:])], axis=1).astype(jnp.bfloat16)

def reference(tokens, norm_gain, query_weight, key_weight, value_weight, sink_logits, conv_in_weight, conv_gate_weight, conv_taps, conv_gain, point_weight, output_gain, output_weight):
    normed = rms_rows(tokens.astype(jnp.float32), norm_gain).astype(jnp.bfloat16)
    queries = jnp.dot(normed, query_weight, preferred_element_type=jnp.float32).astype(jnp.bfloat16)
    key_part = jnp.dot(normed, key_weight, preferred_element_type=jnp.float32).astype(jnp.bfloat16)
    value_part = jnp.dot(normed, value_weight, preferred_element_type=jnp.float32).astype(jnp.bfloat16)
    conv_in = jnp.dot(normed, conv_in_weight, preferred_element_type=jnp.float32)
    conv_gate = jnp.dot(normed, conv_gate_weight, preferred_element_type=jnp.float32)
    gated_rows = (conv_in * jax.nn.sigmoid(conv_gate)).astype(jnp.bfloat16)
    group_size = HEADS // KV_HEADS
    block_count = TOKENS // WINDOW
    head_queries = jnp.transpose(queries.reshape(TOKENS, KV_HEADS, group_size, HEAD_DIM), (1, 0, 2, 3))
    head_keys = jnp.transpose(key_part.reshape(TOKENS, KV_HEADS, HEAD_DIM), (1, 0, 2))
    head_values = jnp.transpose(value_part.reshape(TOKENS, KV_HEADS, HEAD_DIM), (1, 0, 2))
    head_sinks = sink_logits.reshape(KV_HEADS, group_size)
    query_index = lax.broadcasted_iota(jnp.int32, (WINDOW, 2 * WINDOW), 0)
    key_index = lax.broadcasted_iota(jnp.int32, (WINDOW, 2 * WINDOW), 1)
    distance = WINDOW + query_index - key_index
    in_window = (distance >= 0) & (distance < WINDOW)
    block_start = jnp.arange(block_count, dtype=jnp.int32) * WINDOW - WINDOW
    allowed = in_window[None] & (block_start[:, None, None] + key_index[None] >= 0)

    def banded(rows_in):
        padding = jnp.zeros((WINDOW, HEAD_DIM), rows_in.dtype)
        extended = jnp.concatenate([padding, rows_in], axis=0).reshape(block_count + 1, WINDOW, HEAD_DIM)
        return jnp.concatenate([extended[:-1], extended[1:]], axis=1)

    def one_head(operands):
        group_queries, group_keys, group_values, group_sinks = operands
        blocked = group_queries.reshape(block_count, WINDOW, group_size, HEAD_DIM).astype(jnp.float32)
        scores = jnp.einsum('nqgd,njd->ngqj', blocked, banded(group_keys).astype(jnp.float32)) * HEAD_DIM ** (-0.5)
        scores = jnp.where(allowed[:, None], scores, MASKED_SCORE)
        sink_logit = group_sinks[None, :, None, None]
        row_peak = jnp.maximum(lax.optimization_barrier(jnp.max(scores, axis=-1, keepdims=True)), sink_logit)
        raised = jnp.exp(scores - row_peak)
        denominator = lax.optimization_barrier(jnp.sum(raised, axis=-1, keepdims=True)) + jnp.exp(sink_logit - row_peak)
        weights = (raised / denominator).astype(jnp.bfloat16)
        attended = jnp.einsum('ngqj,njd->nqgd', weights.astype(jnp.float32), banded(group_values).astype(jnp.float32))
        return attended.astype(jnp.bfloat16)
    per_head = lax.map(one_head, (head_queries, head_keys, head_values, head_sinks))
    attended = jnp.transpose(per_head, (1, 2, 0, 3, 4)).reshape(TOKENS, HEADS * HEAD_DIM)
    earlier_rows = jnp.zeros((CONV_WIDTH - 1, CHANNELS), jnp.bfloat16)
    convolved = depthwise(gated_rows, earlier_rows, conv_taps)
    activated = layer_activate(convolved, conv_gain)
    pointwise = jnp.dot(activated, point_weight, preferred_element_type=jnp.float32)
    merged = merge_groups(attended, pointwise, output_gain)
    return jnp.dot(merged, output_weight, preferred_element_type=jnp.float32).astype(jnp.bfloat16)
```

```python
import functools

import jax
import jax.numpy as jnp
from jax import lax
from jax.experimental import pallas as pl
from jax.experimental.pallas import tpu as pltpu
from jax.sharding import PartitionSpec as P

HEAD_DIM = 64
WINDOW = 128
CONV_WIDTH = 31
HALO = 32
EPS = 1e-06
MASKED = -1e30
F32 = jnp.float32
BF16 = jnp.bfloat16
MESH = pl.DeviceIdType.MESH


def kernel(
    S, T,
    tok_hbm, ng, qw, kw, vw, sink, iw, gw, taps, cg, pw_hbm, og, ow_hbm,
    out,
    tok, wcat, kws, vws, pw, wfull, qb, kvb, g, a, ar, gr, ext, conv, act, mg,
    lsem, zsend, osend, xsend, ysend, csend, wrecv, hsend, hrecv, asend, arecv, gsend, grecv,
):
    s, t = lax.axis_index("sp"), lax.axis_index("tp")
    R, D = tok.shape
    Q = R // T
    Kl = ow_hbm.shape[0]
    Y, Z = T // 2, S // 2
    z, x = s // 2, lax.rem(s, 2)
    y, c = t // 2, lax.rem(t, 2)
    cw = D // T
    CC = g.shape[1]
    HW = a.shape[1]

    own = pl.ds(pl.multiple_of(s * Kl, Kl), Kl)
    loads = [pltpu.make_async_copy(ow_hbm, wfull.at[own], lsem.at[0])]
    loads += [
        pltpu.make_async_copy(qw, wcat.at[:, 0:HW], lsem.at[1]),
        pltpu.make_async_copy(kw, kws, lsem.at[2]),
        pltpu.make_async_copy(vw, vws, lsem.at[3]),
        pltpu.make_async_copy(iw, wcat.at[:, 2 * HW : 2 * HW + CC], lsem.at[4]),
        pltpu.make_async_copy(gw, wcat.at[:, 2 * HW + CC : 2 * HW + 2 * CC], lsem.at[5]),
        pltpu.make_async_copy(pw_hbm, pw, lsem.at[6]),
    ]
    tloads = [
        pltpu.make_async_copy(tok_hbm.at[q * Q : (q + 1) * Q], tok.at[q * Q : (q + 1) * Q], lsem.at[7 + q])
        for q in range(T)
    ]
    loads[0].start()
    tloads[T - 1].start()
    for i in range(1, 6):
        loads[i].start()
    for q in range(T - 2, -1, -1):
        tloads[q].start()
    loads[6].start()

    bar = pltpu.get_barrier_semaphore()

    def hello(ds_, dt_):
        pl.semaphore_signal(bar, inc=1, device_id=(ds_, dt_), device_id_type=MESH)

    for d in range(1, T):
        hello(s, lax.rem(t + d, T))
    hello(s + 1 - 2 * x, t)
    for step in (1, 2):
        @pl.when(s >= step)
        def _():
            hello(s - step, t)

        @pl.when(s + step < S)
        def _():
            hello(s + step, t)

    peers = T
    for step in (1, 2):
        peers = peers + jnp.where(s >= step, 1, 0) + jnp.where(s + step < S, 1, 0)
    pl.semaphore_wait(bar, peers)

    def piece(sh, col):
        return wfull.at[
            pl.ds(pl.multiple_of(sh * Kl, Kl), Kl), pl.ds(pl.multiple_of(col * cw, cw), cw)
        ]

    def send(sh, col, ds_, dt_, sem):
        ref = piece(sh, col)
        pltpu.make_async_remote_copy(
            src_ref=ref, dst_ref=ref, send_sem=sem, recv_sem=wrecv.at[sh, col],
            device_id=(ds_, dt_), device_id_type=MESH,
        ).start()

    def got(sh, col):
        ref = piece(sh, col)
        pltpu.make_async_copy(ref, ref, wrecv.at[sh, col]).wait()

    def sent(sem):
        ref = piece(0, 0)
        pltpu.make_async_copy(ref, ref, sem).wait()

    mycol = c * Y + y
    other_x = s + 1 - 2 * x
    sib = y * 2 + 1 - c

    def ycol(k):
        return c * Y + lax.rem(y + k, Y)

    def both(d):
        return ((z >= d, z - d, z + 1 < Z, 2), (z + d < Z, z + d, z >= 1, -2))

    def z_own():
        send(s, mycol, other_x, t, xsend.at[z])
        for k in range(Y):
            @pl.when(z + 1 < Z)
            def _():
                send(s, ycol(k), s + 2, t, zsend.at[z, k])

            @pl.when(z >= 1)
            def _():
                send(s, ycol(k), s - 2, t, osend.at[k])

    def z_step(d, k):
        for ok, zz, more, hop in both(d):
            @pl.when(ok)
            def _():
                sh = zz * 2 + x
                got(sh, ycol(k))

                @pl.when(more)
                def _():
                    send(sh, ycol(k), s + hop, t, zsend.at[zz, k])

                if k == 0:
                    send(sh, mycol, other_x, t, xsend.at[zz])
                send(sh, ycol(k), s, sib, csend.at[zz, k])

    def x_one(zz):
        sh = zz * 2 + 1 - x
        got(sh, mycol)
        for k in range(1, Y):
            send(sh, mycol, s, lax.rem(y + k, Y) * 2 + c, ysend.at[zz, k - 1])
        send(sh, mycol, s, sib, csend.at[zz, Y])

    def y_one(zz):
        sh = zz * 2 + 1 - x
        for k in range(1, Y):
            got(sh, ycol(k))
            send(sh, ycol(k), s, sib, csend.at[zz, Y + k])

    def at_distance(d, one):
        if d == 0:
            one(z)
        else:
            for ok, zz, _, _ in both(d):
                @pl.when(ok)
                def _():
                    one(zz)

    events = [
        functools.partial(z_step, 1, 0),
        functools.partial(at_distance, 0, x_one),
    ]
    for k in range(1, Y):
        events.append(functools.partial(z_step, 1, k))
    for d in range(2, Z + 2):
        if d < Z:
            events.append(functools.partial(z_step, d, 0))
        if d - 1 < Z:
            events.append(functools.partial(at_distance, d - 1, x_one))
        events.append(functools.partial(at_distance, d - 2, y_one))
        if d < Z:
            for k in range(1, Y):
                events.append(functools.partial(z_step, d, k))

    loads[0].wait()
    z_own()

    for i in range(1, 6):
        loads[i].wait()
    wcat[:, HW : 2 * HW] = jnp.concatenate([kws[...], vws[...]], axis=1)

    def send_gated(q):
        rows = pl.ds(q * Q, HALO + Q)

        @pl.when(t != q)
        def _():
            pltpu.make_async_remote_copy(
                src_ref=g.at[rows], dst_ref=gr.at[t], send_sem=gsend.at[q], recv_sem=grecv.at[t],
                device_id=(s, q), device_id_type=MESH,
            ).start()

    def halo(ref, n, i):
        return pltpu.make_async_remote_copy(
            src_ref=ref.at[pl.ds(R, n)], dst_ref=ref.at[pl.ds(0, n)],
            send_sem=hsend.at[i], recv_sem=hrecv.at[i],
            device_id=(lax.rem(s + 1, S), t), device_id_type=MESH,
        )

    def run(n):
        for _ in range(n):
            if events:
                events.pop(0)()

    for q in range(T - 1, -1, -1):
        tloads[q].wait()
        xs = tok[q * Q : (q + 1) * Q, :].astype(F32)
        scale = lax.rsqrt(jnp.mean(xs * xs, axis=-1, keepdims=True) + EPS)
        normed = (xs * scale * ng[...]).astype(BF16)
        p = jnp.dot(normed, wcat[...], preferred_element_type=F32)
        qb[q * Q : (q + 1) * Q, :] = (p[:, :HW] * HEAD_DIM ** (-0.5)).astype(BF16)
        kvb[WINDOW + q * Q : WINDOW + (q + 1) * Q, :] = p[:, HW : 2 * HW].astype(BF16)
        g[HALO + q * Q : HALO + (q + 1) * Q, :] = (
            p[:, 2 * HW : 2 * HW + CC] * jax.nn.sigmoid(p[:, 2 * HW + CC :])
        ).astype(BF16)
        if q == T - 1:
            @pl.when(s + 1 < S)
            def _():
                halo(kvb, WINDOW, 0).start()
                halo(g, HALO, 1).start()
        else:
            send_gated(q + 1)
        if q == T - 3:
            run(1)

    @pl.when(s == 0)
    def _():
        kvb[0:WINDOW, :] = jnp.zeros((WINDOW, kvb.shape[1]), BF16)
        g[0:HALO, :] = jnp.zeros((HALO, CC), BF16)

    @pl.when(s > 0)
    def _():
        halo(kvb, WINDOW, 0).wait_recv()
        halo(g, HALO, 1).wait_recv()

    send_gated(0)
    run(2)

    row = lax.broadcasted_iota(jnp.int32, (2 * WINDOW, 2 * WINDOW), 0)
    col = lax.broadcasted_iota(jnp.int32, (2 * WINDOW, 2 * WINDOW), 1)
    dist = WINDOW + lax.rem(row, WINDOW) - col
    inside = (dist >= 0) & (dist < WINDOW)
    head = lax.broadcasted_iota(jnp.int32, (2 * WINDOW, 1), 0) < WINDOW
    sinks = jnp.where(head, sink[0], sink[1])
    for i in range(T):
        q = lax.rem(t + 1 + i, T)
        for b in range(Q // WINDOW):
            base = pl.multiple_of(q * Q + b * WINDOW, WINDOW)
            rows = qb[pl.ds(base, WINDOW), :]
            kv = kvb[pl.ds(base, 2 * WINDOW), :]
            q2 = jnp.concatenate([rows[:, :HEAD_DIM], rows[:, HEAD_DIM:]], axis=0)
            sc = lax.dot_general(
                q2, kv[:, :HEAD_DIM], (((1,), (1,)), ((), ())), preferred_element_type=F32
            )
            low = jnp.where((s == 0) & (base == 0), WINDOW, 0)
            sc = jnp.where(inside & (col >= low), sc, MASKED)
            top = jnp.maximum(jnp.max(sc, axis=-1, keepdims=True), sinks)
            e = jnp.exp(sc - top)
            den = jnp.sum(e, axis=-1, keepdims=True) + jnp.exp(sinks - top)
            w = (e * (1.0 / den)).astype(BF16)
            o = jnp.dot(w, kv[:, HEAD_DIM:], preferred_element_type=F32).astype(BF16)
            a[pl.ds(base, WINDOW), :] = jnp.concatenate([o[:WINDOW], o[WINDOW:]], axis=1)
        if i < T - 1:
            pltpu.make_async_remote_copy(
                src_ref=a.at[pl.ds(pl.multiple_of(q * Q, Q), Q)], dst_ref=ar.at[t],
                send_sem=asend.at[i], recv_sem=arecv.at[t],
                device_id=(s, q), device_id_type=MESH,
            ).start()
        run(1)
    mine = pl.multiple_of(t * Q, Q)
    ar[t] = a[pl.ds(mine, Q), :]
    gr[t] = g[pl.ds(mine, HALO + Q), :]
    run(1)

    first = HALO - (CONV_WIDTH - 1)
    for d in range(1, T):
        p = lax.rem(t + d, T)
        pltpu.make_async_copy(gr.at[p], gr.at[p], grecv.at[p]).wait()
    total = jnp.zeros((Q, 1), F32)
    for p in range(T):
        ext[p] = gr[p].astype(F32)
        acc = jnp.zeros((Q, CC), F32)
        tp = taps[:, p * CC : (p + 1) * CC].astype(F32)
        for k in range(CONV_WIDTH):
            acc = acc + tp[k : k + 1] * ext[p, first + k : first + k + Q, :]
        rounded = acc.astype(BF16)
        conv[:, p * CC : (p + 1) * CC] = rounded
        if p == 1:
            run(1)
    run(1)
    cv = conv[...].astype(F32)
    cen = cv - jnp.mean(cv, axis=-1, keepdims=True)
    norm = cen * lax.rsqrt(jnp.mean(cen * cen, axis=-1, keepdims=True) + EPS) * cg[...]
    act[...] = (norm * jax.nn.sigmoid(norm)).astype(BF16)
    loads[6].wait()
    pt = jnp.dot(act[...], pw[...], preferred_element_type=F32)
    AW = T * HW
    mg[:, AW:] = (
        pt * lax.rsqrt(jnp.mean(pt * pt, axis=-1, keepdims=True) + EPS) * og[:, AW:]
    ).astype(BF16)
    run(1)
    for d in range(1, T):
        p = lax.rem(t + d, T)
        pltpu.make_async_copy(ar.at[p], ar.at[p], arecv.at[p]).wait()
    heads = jnp.concatenate([ar[p] for p in range(T)], axis=1).astype(F32)
    mg[:, :AW] = (
        heads * lax.rsqrt(jnp.mean(heads * heads, axis=-1, keepdims=True) + EPS) * og[:, :AW]
    ).astype(BF16)

    run(len(events))
    scol = [(1 - c) * Y + k for k in range(Y)]
    for d in range(Z):
        def rest(zz):
            for k in range(Y):
                if d > 0:
                    got(zz * 2 + x, scol[k])
                got(zz * 2 + 1 - x, scol[k])
        at_distance(d, rest)

    nb = 512
    for n in range(D // nb):
        out[:, n * nb : (n + 1) * nb] = jnp.dot(
            mg[...], wfull[:, n * nb : (n + 1) * nb], preferred_element_type=F32
        ).astype(BF16)

    sent(xsend.at[z])
    for k in range(Y):
        @pl.when(z + 1 < Z)
        def _():
            sent(zsend.at[z, k])

        @pl.when(z >= 1)
        def _():
            sent(osend.at[k])

    for d in range(Z):
        if d > 0:
            for ok, zz, more, _ in both(d):
                @pl.when(ok)
                def _():
                    for k in range(Y):
                        @pl.when(more)
                        def _():
                            sent(zsend.at[zz, k])
                        sent(csend.at[zz, k])
                    sent(xsend.at[zz])

        def done(zz):
            for k in range(1, Y):
                sent(ysend.at[zz, k - 1])
                sent(csend.at[zz, Y + k])
            sent(csend.at[zz, Y])
        at_distance(d, done)

    @pl.when(s + 1 < S)
    def _():
        halo(kvb, WINDOW, 0).wait_send()
        halo(g, HALO, 1).wait_send()

    for q in range(T):
        @pl.when(t != q)
        def _():
            pltpu.make_async_copy(gr.at[0], gr.at[0], gsend.at[q]).wait()
    for i in range(T - 1):
        pltpu.make_async_copy(ar.at[0], ar.at[0], asend.at[i]).wait()


def solution(mesh):
    S, T = mesh.shape["sp"], mesh.shape["tp"]

    def step(
        tokens, norm_gain, query_weight, key_weight, value_weight, sink_logits, conv_in_weight,
        conv_gate_weight, conv_taps, conv_gain, point_weight, output_gain, output_weight,
    ):
        R, D = tokens.shape
        Q = R // T
        HW, KW, CC = query_weight.shape[1], key_weight.shape[1], conv_in_weight.shape[1]
        C = point_weight.shape[0]
        MIX = output_gain.shape[0]
        Y, Z = T // 2, S // 2
        hbm = pl.BlockSpec(memory_space=pl.ANY)
        vmem = pl.BlockSpec(memory_space=pltpu.VMEM)
        smem = pl.BlockSpec(memory_space=pltpu.SMEM)
        dma = pltpu.SemaphoreType.DMA
        return pl.pallas_call(
            functools.partial(kernel, S, T),
            out_shape=jax.ShapeDtypeStruct((Q, D), BF16),
            in_specs=[hbm, vmem, hbm, hbm, hbm, smem, hbm, hbm, vmem, vmem, hbm, vmem, hbm],
            out_specs=vmem,
            scratch_shapes=[
                pltpu.VMEM((R, D), BF16),
                pltpu.VMEM((D, HW + 2 * KW + 2 * CC), BF16),
                pltpu.VMEM((D, KW), BF16),
                pltpu.VMEM((D, KW), BF16),
                pltpu.VMEM((C, C), BF16),
                pltpu.VMEM((MIX, D), BF16),
                pltpu.VMEM((R, HW), BF16),
                pltpu.VMEM((R + WINDOW, 2 * KW), BF16),
                pltpu.VMEM((R + HALO, CC), BF16),
                pltpu.VMEM((R, HW), BF16),
                pltpu.VMEM((T, Q, HW), BF16),
                pltpu.VMEM((T, Q + HALO, CC), BF16),
                pltpu.VMEM((T, Q + HALO, CC), F32),
                pltpu.VMEM((Q, C), BF16),
                pltpu.VMEM((Q, C), BF16),
                pltpu.VMEM((Q, MIX), BF16),
                dma((7 + T,)),
                dma((Z, Y)),
                dma((Y,)),
                dma((Z,)),
                dma((Z, Y - 1)),
                dma((Z, 2 * Y)),
                dma((S, T)),
                dma((2,)),
                dma((2,)),
                dma((T,)),
                dma((T,)),
                dma((T,)),
                dma((T,)),
            ],
            compiler_params=pltpu.CompilerParams(
                collective_id=0, has_side_effects=True, vmem_limit_bytes=56 * 1024 * 1024
            ),
        )(
            tokens, norm_gain[None], query_weight, key_weight, value_weight, sink_logits,
            conv_in_weight, conv_gate_weight, conv_taps, conv_gain[None], point_weight,
            output_gain[None], output_weight,
        )

    in_specs = (
        P("sp", None), P(), P(None, "tp"), P(None, "tp"), P(None, "tp"), P("tp"), P(None, "tp"),
        P(None, "tp"), P(), P(), P(), P(), P("sp", None),
    )
    return jax.shard_map(
        step, mesh=mesh, in_specs=in_specs, out_specs=P(("sp", "tp"), None), check_vma=False
    )
```

```python
import functools

import jax
import jax.numpy as jnp
from jax import lax
from jax.experimental import pallas as pl
from jax.experimental.pallas import tpu as pltpu
from jax.sharding import PartitionSpec as P

HEAD_DIM = 64
WINDOW = 128
CONV_WIDTH = 31
HALO = 32
EPS = 1e-06
MASKED = -1e30
F32 = jnp.float32
BF16 = jnp.bfloat16
MESH = pl.DeviceIdType.MESH


def kernel(
    S, T,
    tok_hbm, ng, qw, kw, vw, sink, iw, gw, taps, cg, pw_hbm, og, ow_hbm,
    out,
    tok, wcat, kvs, pw, wfull, qb, kvb, g, a, ar, gr, ext, conv, act, mg,
    lsem, zsend, osend, psend, xsend, ysend, csend, wrecv, hsend, hrecv, asend, arecv, gsend, grecv,
):
    s, t = lax.axis_index("sp"), lax.axis_index("tp")
    R, D = tok.shape
    Q = R // T
    Kl = ow_hbm.shape[0]
    Y, Z = T // 2, S // 2
    z, x = s // 2, lax.rem(s, 2)
    y, c = t // 2, lax.rem(t, 2)
    CC = g.shape[1]
    HW = a.shape[1]

    own = pl.ds(pl.multiple_of(s * Kl, Kl), Kl)
    loads = [pltpu.make_async_copy(ow_hbm, wfull.at[own], lsem.at[0])]
    loads += [
        pltpu.make_async_copy(qw, wcat.at[:, 0:HW], lsem.at[1]),
        pltpu.make_async_copy(kw, kvs.at[0 : kw.shape[0]], lsem.at[2]),
        pltpu.make_async_copy(vw, kvs.at[kw.shape[0] : 2 * kw.shape[0]], lsem.at[3]),
        pltpu.make_async_copy(iw, wcat.at[:, 2 * HW : 2 * HW + CC], lsem.at[4]),
        pltpu.make_async_copy(gw, wcat.at[:, 2 * HW + CC : 2 * HW + 2 * CC], lsem.at[5]),
        pltpu.make_async_copy(pw_hbm, pw, lsem.at[6]),
    ]
    tloads = [
        pltpu.make_async_copy(tok_hbm.at[q * Q : (q + 1) * Q], tok.at[q * Q : (q + 1) * Q], lsem.at[7 + q])
        for q in range(T)
    ]
    loads[0].start()
    tloads[T - 1].start()
    for i in range(1, 6):
        loads[i].start()
    for q in range(T - 2, -1, -1):
        tloads[q].start()
    loads[6].start()

    bar = pltpu.get_barrier_semaphore()

    def hello(ds_, dt_):
        pl.semaphore_signal(bar, inc=1, device_id=(ds_, dt_), device_id_type=MESH)

    for d in range(1, T):
        hello(s, lax.rem(t + d, T))
    hello(s + 1 - 2 * x, t)
    for step in (1, 2):
        @pl.when(s >= step)
        def _():
            hello(s - step, t)

        @pl.when(s + step < S)
        def _():
            hello(s + step, t)

    peers = T
    for step in (1, 2):
        peers = peers + jnp.where(s >= step, 1, 0) + jnp.where(s + step < S, 1, 0)
    pl.semaphore_wait(bar, peers)

    half, wide = D // 2, D // 4
    narrow = wide // Y
    other_x = s + 1 - 2 * x
    sib = y * 2 + 1 - c

    def piece(sh, cc, j):
        rows = pl.ds(pl.multiple_of(sh * Kl, Kl), Kl)
        if j is None:
            return wfull.at[rows, pl.ds(pl.multiple_of(cc * half, wide), wide)]
        return wfull.at[rows, pl.ds(pl.multiple_of(cc * half + wide + j * narrow, narrow), narrow)]

    def slot(cc, j):
        return cc * (Y + 1) + (0 if j is None else 1 + j)

    def send(sh, j, ds_, dt_, sem):
        ref = piece(sh, c, j)
        pltpu.make_async_remote_copy(
            src_ref=ref, dst_ref=ref, send_sem=sem, recv_sem=wrecv.at[sh, slot(c, j)],
            device_id=(ds_, dt_), device_id_type=MESH,
        ).start()

    def got(sh, cc, j):
        ref = piece(sh, cc, j)
        pltpu.make_async_copy(ref, ref, wrecv.at[sh, slot(cc, j)]).wait()

    def sent(j, sem):
        ref = piece(0, 0, j)
        pltpu.make_async_copy(ref, ref, sem).wait()

    def yplane(k):
        return lax.rem(y + k, Y)

    def both(d):
        return ((z >= d, z - d, z + 1 < Z, 2), (z + d < Z, z + d, z >= 1, -2))

    def z_both(sh, j, i):
        @pl.when(z + 1 < Z)
        def _():
            send(sh, j, s + 2, t, zsend.at[z, i])

        @pl.when(z >= 1)
        def _():
            send(sh, j, s - 2, t, osend.at[i])

    def across_y(sh, zz, i):
        for k in range(1, Y):
            send(sh, y, s, yplane(k) * 2 + c, ysend.at[zz, i * (Y - 1) + k - 1])

    def z_own():
        send(s, y, other_x, t, psend.at[0])
        z_both(s, None, 0)
        send(s, None, other_x, t, xsend.at[z])
        z_both(s, y, 1)

    def crossed():
        got(other_x, c, y)
        z_both(other_x, y, 2)
        across_y(other_x, z, 1)
        send(other_x, y, s, sib, csend.at[z, Y + 2])

    def z_step(d, i):
        for ok, zz, more, hop in both(d):
            @pl.when(ok)
            def _():
                sh = zz * 2 + (1 - x if i == 2 else x)
                j = None if i == 0 else y
                got(sh, c, j)

                @pl.when(more)
                def _():
                    send(sh, j, s + hop, t, zsend.at[zz, i])

                if i == 0:
                    send(sh, j, other_x, t, xsend.at[zz])
                    send(sh, j, s, sib, csend.at[zz, 0])
                else:
                    across_y(sh, zz, i - 1)
                    send(sh, j, s, sib, csend.at[zz, (i - 1) * (Y + 1) + 1])

    def at_distance(d, one):
        if d == 0:
            one(z)
        else:
            for ok, zz, _, _ in both(d):
                @pl.when(ok)
                def _():
                    one(zz)

    def x_one(zz):
        sh = zz * 2 + 1 - x
        got(sh, c, None)
        send(sh, None, s, sib, csend.at[zz, Y + 1])

    def y_one(d):
        def one(zz):
            for i in ((1,) if d == 0 else (0, 1)):
                sh = zz * 2 + (x if i == 0 else 1 - x)
                for k in range(1, Y):
                    got(sh, c, yplane(k))
                    send(sh, yplane(k), s, sib, csend.at[zz, i * (Y + 1) + 1 + k])
        at_distance(d, one)

    events = [crossed]
    for d in range(1, Z + 1):
        if d < Z:
            for i in range(3):
                events.append(functools.partial(z_step, d, i))
        events.append(functools.partial(at_distance, d - 1, x_one))
        events.append(functools.partial(y_one, d - 1))

    loads[0].wait()
    z_own()

    for i in range(1, 6):
        loads[i].wait()
    wcat[:, HW : 2 * HW] = kvs[...].T

    def send_gated(q):
        rows = pl.ds(q * Q, HALO + Q)

        @pl.when(t != q)
        def _():
            pltpu.make_async_remote_copy(
                src_ref=g.at[rows], dst_ref=gr.at[t], send_sem=gsend.at[q], recv_sem=grecv.at[t],
                device_id=(s, q), device_id_type=MESH,
            ).start()

    def halo(ref, n, i):
        return pltpu.make_async_remote_copy(
            src_ref=ref.at[pl.ds(R, n)], dst_ref=ref.at[pl.ds(0, n)],
            send_sem=hsend.at[i], recv_sem=hrecv.at[i],
            device_id=(lax.rem(s + 1, S), t), device_id_type=MESH,
        )

    def run(n):
        for _ in range(n):
            if events:
                events.pop(0)()

    for q in range(T - 1, -1, -1):
        tloads[q].wait()
        xs = tok[q * Q : (q + 1) * Q, :].astype(F32)
        scale = lax.rsqrt(jnp.mean(xs * xs, axis=-1, keepdims=True) + EPS)
        normed = (xs * scale * ng[...]).astype(BF16)
        p = jnp.dot(normed, wcat[...], preferred_element_type=F32)
        qb[q * Q : (q + 1) * Q, :] = (p[:, :HW] * HEAD_DIM ** (-0.5)).astype(BF16)
        kvb[WINDOW + q * Q : WINDOW + (q + 1) * Q, :] = p[:, HW : 2 * HW].astype(BF16)
        g[HALO + q * Q : HALO + (q + 1) * Q, :] = (
            p[:, 2 * HW : 2 * HW + CC] * jax.nn.sigmoid(p[:, 2 * HW + CC :])
        ).astype(BF16)
        if q == T - 1:
            @pl.when(s + 1 < S)
            def _():
                halo(kvb, WINDOW, 0).start()
                halo(g, HALO, 1).start()
        else:
            send_gated(q + 1)
        run(1 if q == T - 1 else 2 if q < T - 2 else 1)

    @pl.when(s == 0)
    def _():
        kvb[0:WINDOW, :] = jnp.zeros((WINDOW, kvb.shape[1]), BF16)
        g[0:HALO, :] = jnp.zeros((HALO, CC), BF16)

    @pl.when(s > 0)
    def _():
        halo(kvb, WINDOW, 0).wait_recv()
        halo(g, HALO, 1).wait_recv()

    send_gated(0)

    row = lax.broadcasted_iota(jnp.int32, (2 * WINDOW, 2 * WINDOW), 0)
    col = lax.broadcasted_iota(jnp.int32, (2 * WINDOW, 2 * WINDOW), 1)
    dist = WINDOW + lax.rem(row, WINDOW) - col
    inside = (dist >= 0) & (dist < WINDOW)
    head = lax.broadcasted_iota(jnp.int32, (2 * WINDOW, 1), 0) < WINDOW
    sinks = jnp.where(head, sink[0], sink[1])
    for i in range(T):
        q = lax.rem(t + 1 + i, T)
        for b in range(Q // WINDOW):
            base = pl.multiple_of(q * Q + b * WINDOW, WINDOW)
            rows = qb[pl.ds(base, WINDOW), :]
            kv = kvb[pl.ds(base, 2 * WINDOW), :]
            q2 = jnp.concatenate([rows[:, :HEAD_DIM], rows[:, HEAD_DIM:]], axis=0)
            sc = lax.dot_general(
                q2, kv[:, :HEAD_DIM], (((1,), (1,)), ((), ())), preferred_element_type=F32
            )
            low = jnp.where((s == 0) & (base == 0), WINDOW, 0)
            sc = jnp.where(inside & (col >= low), sc, MASKED)
            top = jnp.maximum(jnp.max(sc, axis=-1, keepdims=True), sinks)
            e = jnp.exp(sc - top)
            den = jnp.sum(e, axis=-1, keepdims=True) + jnp.exp(sinks - top)
            w = (e * (1.0 / den)).astype(BF16)
            o = jnp.dot(w, kv[:, HEAD_DIM:], preferred_element_type=F32).astype(BF16)
            a[pl.ds(base, WINDOW), :] = jnp.concatenate([o[:WINDOW], o[WINDOW:]], axis=1)
        if i < T - 1:
            pltpu.make_async_remote_copy(
                src_ref=a.at[pl.ds(pl.multiple_of(q * Q, Q), Q)], dst_ref=ar.at[t],
                send_sem=asend.at[i], recv_sem=arecv.at[t],
                device_id=(s, q), device_id_type=MESH,
            ).start()
        run(2)
    mine = pl.multiple_of(t * Q, Q)
    ar[t] = a[pl.ds(mine, Q), :]
    gr[t] = g[pl.ds(mine, HALO + Q), :]
    run(1)

    first = HALO - (CONV_WIDTH - 1)
    for d in range(1, T):
        p = lax.rem(t + d, T)
        pltpu.make_async_copy(gr.at[p], gr.at[p], grecv.at[p]).wait()
    total = jnp.zeros((Q, 1), F32)
    for p in range(T):
        ext[p] = gr[p].astype(F32)
        acc = jnp.zeros((Q, CC), F32)
        tp = taps[:, p * CC : (p + 1) * CC].astype(F32)
        for k in range(CONV_WIDTH):
            acc = acc + tp[k : k + 1] * ext[p, first + k : first + k + Q, :]
        rounded = acc.astype(BF16)
        conv[:, p * CC : (p + 1) * CC] = rounded
        if p == 1:
            run(1)
    run(1)
    cv = conv[...].astype(F32)
    cen = cv - jnp.mean(cv, axis=-1, keepdims=True)
    norm = cen * lax.rsqrt(jnp.mean(cen * cen, axis=-1, keepdims=True) + EPS) * cg[...]
    act[...] = (norm * jax.nn.sigmoid(norm)).astype(BF16)
    loads[6].wait()
    pt = jnp.dot(act[...], pw[...], preferred_element_type=F32)
    AW = T * HW
    mg[:, AW:] = (
        pt * lax.rsqrt(jnp.mean(pt * pt, axis=-1, keepdims=True) + EPS) * og[:, AW:]
    ).astype(BF16)
    run(1)
    for d in range(1, T):
        p = lax.rem(t + d, T)
        pltpu.make_async_copy(ar.at[p], ar.at[p], arecv.at[p]).wait()
    heads = jnp.concatenate([ar[p] for p in range(T)], axis=1).astype(F32)
    mg[:, :AW] = (
        heads * lax.rsqrt(jnp.mean(heads * heads, axis=-1, keepdims=True) + EPS) * og[:, :AW]
    ).astype(BF16)

    run(len(events))
    for d in range(Z):
        def rest(zz):
            for j in (None, *range(Y)):
                if d > 0:
                    got(zz * 2 + x, 1 - c, j)
                got(zz * 2 + 1 - x, 1 - c, j)
        at_distance(d, rest)

    nb = 512
    for n in range(D // nb):
        out[:, n * nb : (n + 1) * nb] = jnp.dot(
            mg[...], wfull[:, n * nb : (n + 1) * nb], preferred_element_type=F32
        ).astype(BF16)

    sent(0, psend.at[0])
    for i in range(3):
        j = None if i == 0 else 0

        @pl.when(z + 1 < Z)
        def _():
            sent(j, zsend.at[z, i])

        @pl.when(z >= 1)
        def _():
            sent(j, osend.at[i])

    for d in range(1, Z):
        for ok, zz, more, _ in both(d):
            @pl.when(ok & more)
            def _():
                for i in range(3):
                    sent(None if i == 0 else 0, zsend.at[zz, i])

    for d in range(Z):
        def done(zz):
            sent(None, xsend.at[zz])
            for i in ((1,) if d == 0 else (0, 1)):
                for k in range(1, Y):
                    sent(0, ysend.at[zz, i * (Y - 1) + k - 1])
                for k in range(Y + 1):
                    sent(None if k == 0 else 0, csend.at[zz, i * (Y + 1) + k])
        at_distance(d, done)

    @pl.when(s + 1 < S)
    def _():
        halo(kvb, WINDOW, 0).wait_send()
        halo(g, HALO, 1).wait_send()

    for q in range(T):
        @pl.when(t != q)
        def _():
            pltpu.make_async_copy(gr.at[0], gr.at[0], gsend.at[q]).wait()
    for i in range(T - 1):
        pltpu.make_async_copy(ar.at[0], ar.at[0], asend.at[i]).wait()


def solution(mesh):
    S, T = mesh.shape["sp"], mesh.shape["tp"]

    def step(
        tokens, norm_gain, query_weight, key_weight, value_weight, sink_logits, conv_in_weight,
        conv_gate_weight, conv_taps, conv_gain, point_weight, output_gain, output_weight,
    ):
        R, D = tokens.shape
        Q = R // T
        HW, KW, CC = query_weight.shape[1], key_weight.shape[1], conv_in_weight.shape[1]
        C = point_weight.shape[0]
        MIX = output_gain.shape[0]
        Y, Z = T // 2, S // 2
        hbm = pl.BlockSpec(memory_space=pl.ANY)
        vmem = pl.BlockSpec(memory_space=pltpu.VMEM)
        smem = pl.BlockSpec(memory_space=pltpu.SMEM)
        dma = pltpu.SemaphoreType.DMA
        return pl.pallas_call(
            functools.partial(kernel, S, T),
            out_shape=jax.ShapeDtypeStruct((Q, D), BF16),
            in_specs=[hbm, vmem, hbm, hbm, hbm, smem, hbm, hbm, vmem, vmem, hbm, vmem, hbm],
            out_specs=vmem,
            scratch_shapes=[
                pltpu.VMEM((R, D), BF16),
                pltpu.VMEM((D, HW + 2 * KW + 2 * CC), BF16),
                pltpu.VMEM((2 * KW, D), BF16),
                pltpu.VMEM((C, C), BF16),
                pltpu.VMEM((MIX, D), BF16),
                pltpu.VMEM((R, HW), BF16),
                pltpu.VMEM((R + WINDOW, 2 * KW), BF16),
                pltpu.VMEM((R + HALO, CC), BF16),
                pltpu.VMEM((R, HW), BF16),
                pltpu.VMEM((T, Q, HW), BF16),
                pltpu.VMEM((T, Q + HALO, CC), BF16),
                pltpu.VMEM((T, Q + HALO, CC), F32),
                pltpu.VMEM((Q, C), BF16),
                pltpu.VMEM((Q, C), BF16),
                pltpu.VMEM((Q, MIX), BF16),
                dma((7 + T,)),
                dma((Z, 3)),
                dma((3,)),
                dma((1,)),
                dma((Z,)),
                dma((Z, 2 * (Y - 1))),
                dma((Z, 2 * (Y + 1))),
                dma((S, 2 * (Y + 1))),
                dma((2,)),
                dma((2,)),
                dma((T,)),
                dma((T,)),
                dma((T,)),
                dma((T,)),
            ],
            compiler_params=pltpu.CompilerParams(
                collective_id=0, has_side_effects=True, vmem_limit_bytes=56 * 1024 * 1024
            ),
        )(
            tokens, norm_gain[None], query_weight, key_weight.T, value_weight.T, sink_logits,
            conv_in_weight, conv_gate_weight, conv_taps, conv_gain[None], point_weight,
            output_gain[None], output_weight,
        )

    in_specs = (
        P("sp", None), P(), P(None, "tp"), P(None, "tp"), P(None, "tp"), P("tp"), P(None, "tp"),
        P(None, "tp"), P(), P(), P(), P(), P("sp", None),
    )
    return jax.shard_map(
        step, mesh=mesh, in_specs=in_specs, out_specs=P(("sp", "tp"), None), check_vma=False
    )
```
